256 devices in a mesh: sp: 64 (over z, y, core), tp: 4 (over x).
Axes of the slice: x: 4, y: 4, z: 8, core: 2. Of those that a mesh axis runs over, the one named last changes fastest.
Arguments:
- tokens: bfloat16 [24576, 2048], P(('sp', 'tp')), may hold values from -60 to 60
- query_weight: bfloat16 [2048, 1024], P(None, 'tp'), may hold values from -0.125 to 0.125
- key_weight: bfloat16 [2048, 1024], P(None, 'tp'), may hold values from -0.125 to 0.125
- value_weight: bfloat16 [2048, 1024], P(None, 'tp'), may hold values from -0.125 to 0.125
- outer_gate: bfloat16 [2048, 1024], P(None, 'tp'), may hold values from -0.125 to 0.125
- inner_gate: bfloat16 [2048, 1024], P(None, 'tp'), may hold values from -0.125 to 0.125
- conv_weight: bfloat16 [2048, 1024], P(None, 'tp'), may hold values from -0.125 to 0.125
- conv_taps: bfloat16 [3, 1024], P(None, 'tp'), may hold values from -3 to 3
- gate_sum: float32 [8, 24576], P('tp'), may hold values from -1412 to 0, as said below
- head_gain: bfloat16 [1024], P('tp'), may hold values from 0.099609375 to 1.8984375
- channel_gain: bfloat16 [1024], P('tp'), may hold values from 0.099609375 to 1.8984375
- attention_out: bfloat16 [1024, 2048], P('tp'), may hold values from -0.125 to 0.125
- channel_out: bfloat16 [1024, 2048], P('tp'), may hold values from -0.125 to 0.125
Outputs:
- mixed_out: bfloat16 [24576, 2048], P(('sp', 'tp'))
The draws below stay inside these ranges and needn't reach their ends.
Inputs may be any that keep to these rules, and one draw needn't show every extreme that they name: gate_sum[h, t] never rises with t.
All inputs are finite; a program needn't handle non-finite values.
Results may differ from the reference program's by a relative error of at most 0.015.
Values may be sent and summed in bfloat16 or wider, within the bound.
No kernel may reach another device: no remote copies, remote signals or barrier semaphores. Data moves between devices by JAX's collectives and lax.ppermute only.
A program may use at most 192 MiB of HBM per device.

```python
import math
import jax
import jax.numpy as jnp
from jax import lax

D = 2048
ATTENTION_HEADS = 8
HEAD = 128
KTAP = 3
TOK_DEV = 384
AW = 1024
CW = 1024
SEQUENCE_TOKENS = 24576


def draw_tokens(key, part):
    key_sequence = jax.random.split(jax.random.fold_in(key, 7), 6)
    return jnp.clip(jax.random.normal(key_sequence[5], (SEQUENCE_TOKENS, D), jnp.float32), -6.0, 6.0).astype(jnp.bfloat16)


def draw_gate_sum(key, part):
    key_sequence = jax.random.split(jax.random.fold_in(key, 11), 5)
    head_order = jax.random.permutation(key_sequence[0], ATTENTION_HEADS)
    quick_decay_heads = head_order < ATTENTION_HEADS // 2
    jitter = jax.random.uniform(key_sequence[1], (ATTENTION_HEADS, SEQUENCE_TOKENS), jnp.float32, 0.25, 1.75)
    block_rates = jnp.exp(jax.random.uniform(key_sequence[2], (SEQUENCE_TOKENS // TOK_DEV,), jnp.float32, math.log(0.5), math.log(2.0)))
    position_rates = jnp.repeat(block_rates, TOK_DEV)
    forget_rates = jnp.where(quick_decay_heads[:, None], 6.0 / TOK_DEV, 0.5 / SEQUENCE_TOKENS) * jitter * position_rates[None, :]
    cluster_position = jax.random.randint(key_sequence[3], (ATTENTION_HEADS, 3), 0, SEQUENCE_TOKENS)
    cluster_length = jax.random.uniform(key_sequence[4], (ATTENTION_HEADS, 3), jnp.float32, math.log(0.5), math.log(0.8))
    token_positions = jnp.arange(SEQUENCE_TOKENS)
    cluster_match = token_positions[None, None, :] == cluster_position[:, :, None]
    token_clusters = jnp.sum(jnp.where(cluster_match, cluster_length[:, :, None], 0.0), axis=1)
    token_clusters = jnp.where(quick_decay_heads[:, None], 0.0, token_clusters)
    return jnp.cumsum(token_clusters - forget_rates, axis=1)


def shard_levels(rng, extent, cuts, least, largest):
    factor_of, own = 1.0, jax.random.fold_in(rng, 6)
    for dim, shards_of in cuts:
        heights = jnp.exp(jax.random.uniform(jax.random.fold_in(own, dim), (shards_of,), jnp.float32, least / len(cuts), largest / len(cuts)))
        factor_of = factor_of * jnp.repeat(heights, extent[dim] // shards_of).reshape([-1 if axis == dim else 1 for axis in range(len(extent))])
    return factor_of


def scatter_about(rng, extent, deviation, most, cuts=(), held_as=jnp.bfloat16):
    level = shard_levels(rng, extent, cuts, -0.22, 0.18) if cuts else 1.0
    array = jax.random.normal(rng, extent, jnp.float32) * deviation * level
    return jnp.minimum(jnp.maximum(array, -most), most).astype(held_as)


def setup_inputs(seed: int = 0) -> dict:
    keys = jax.random.split(jax.random.key(seed), 14)
    tokens = draw_tokens(jax.random.fold_in(keys[13], 71), 0)
    query_weight = scatter_about(keys[1], (D, AW), D ** -0.5, 0.125, ((1, 4),))
    key_weight = scatter_about(keys[2], (D, AW), D ** -0.5, 0.125, ((1, 4),))
    value_weight = scatter_about(keys[3], (D, AW), D ** -0.5, 0.125, ((1, 4),))
    outer_gate = scatter_about(keys[4], (D, CW), D ** -0.5, 0.125, ((1, 4),))
    inner_gate = scatter_about(keys[5], (D, CW), D ** -0.5, 0.125, ((1, 4),))
    conv_weight = scatter_about(keys[6], (D, CW), D ** -0.5, 0.125, ((1, 4),))
    conv_taps = scatter_about(keys[7], (KTAP, CW), 0.577, 3.0, ((1, 4),))
    gate_sum = draw_gate_sum(jax.random.fold_in(keys[13], 71), 0)
    head_gain = jnp.clip(1.0 + 0.18 * jax.random.normal(keys[9], (AW,), jnp.float32), 0.099609375, 1.8984375).astype(jnp.bfloat16)
    channel_gain = jnp.clip(1.0 + 0.18 * jax.random.normal(keys[10], (CW,), jnp.float32), 0.099609375, 1.8984375).astype(jnp.bfloat16)
    attention_out = scatter_about(keys[11], (AW, D), (AW + CW) ** -0.5, 0.125, ((0, 4),))
    channel_out = scatter_about(keys[12], (CW, D), (AW + CW) ** -0.5, 0.125, ((0, 4),))
    return {"tokens": tokens, "query_weight": query_weight, "key_weight": key_weight, "value_weight": value_weight, "outer_gate": outer_gate, "inner_gate": inner_gate, "conv_weight": conv_weight, "conv_taps": conv_taps, "gate_sum": gate_sum, "head_gain": head_gain, "channel_gain": channel_gain, "attention_out": attention_out, "channel_out": channel_out}


def project_rows(tokens, weight):
    return jnp.dot(tokens, weight, preferred_element_type=jnp.float32).astype(jnp.bfloat16)

def head_norm(values, gain_vector):
    row_count = values.shape[0]
    shaped = values.reshape(row_count, -1, HEAD)
    shaped = shaped * lax.rsqrt(lax.optimization_barrier(jnp.mean(shaped * shaped, axis=-1, keepdims=True)) + 1e-06)
    return (shaped.reshape(row_count, -1) * gain_vector.astype(jnp.float32)).astype(jnp.bfloat16)

def reference(tokens, query_weight, key_weight, value_weight, outer_gate, inner_gate, conv_weight, conv_taps, gate_sum, head_gain, channel_gain, attention_out, channel_out):
    queries = project_rows(tokens, query_weight)
    keys_all = project_rows(tokens, key_weight)
    values_all = project_rows(tokens, value_weight)
    gate_outer = project_rows(tokens, outer_gate)
    gate_inner = project_rows(tokens, inner_gate)
    conv_input = project_rows(tokens, conv_weight)
    mixed_in = (gate_inner.astype(jnp.float32) * conv_input.astype(jnp.float32)).astype(jnp.bfloat16)
    padded = jnp.concatenate([jnp.zeros((KTAP - 1, CW), jnp.float32), mixed_in.astype(jnp.float32)], axis=0)
    summed = jnp.zeros((SEQUENCE_TOKENS, CW), jnp.float32)
    for offset in range(KTAP):
        summed = summed + conv_taps[offset].astype(jnp.float32) * padded[offset:offset + SEQUENCE_TOKENS]
    conv_out = gate_outer.astype(jnp.float32) * summed
    block_rows = math.gcd(SEQUENCE_TOKENS, 512)
    query_heads = queries.reshape(SEQUENCE_TOKENS, ATTENTION_HEADS, HEAD).astype(jnp.float32)
    key_heads = keys_all.reshape(SEQUENCE_TOKENS, ATTENTION_HEADS, HEAD).astype(jnp.float32)
    value_heads = values_all.reshape(SEQUENCE_TOKENS, ATTENTION_HEADS, HEAD).astype(jnp.float32)
    score_scale = HEAD ** (-0.5)
    token_positions = jnp.arange(SEQUENCE_TOKENS, dtype=jnp.int32)

    def attend(block_index):
        first_row = (block_index * block_rows).astype(jnp.int32)
        query_block = lax.dynamic_slice_in_dim(query_heads, first_row, block_rows, 0)
        gate_block = lax.dynamic_slice_in_dim(gate_sum, first_row, block_rows, 1)
        query_pos = first_row + jnp.arange(block_rows, dtype=jnp.int32)
        logits = jnp.einsum('qhd,khd->qhk', query_block, key_heads) * score_scale
        logits = logits + gate_block.T[:, :, None] - gate_sum[None, :, :]
        allowed = (token_positions[None, :] <= query_pos[:, None])[:, None, :]
        logits = jnp.where(allowed, logits, -jnp.inf)
        peak = lax.optimization_barrier(jnp.max(logits, axis=-1, keepdims=True))
        weights = jnp.exp(logits - peak)
        total = lax.optimization_barrier(jnp.sum(weights, axis=-1))
        rounded = lax.optimization_barrier(weights.astype(jnp.bfloat16))
        mixed = jnp.einsum('qhk,khd->qhd', rounded.astype(jnp.float32), value_heads)
        return mixed / total[..., None]
    blocks = lax.map(attend, jnp.arange(SEQUENCE_TOKENS // block_rows, dtype=jnp.int32))
    attention = blocks.reshape(SEQUENCE_TOKENS, ATTENTION_HEADS * HEAD)
    head_normed = head_norm(attention, head_gain)
    group_normed = head_norm(conv_out, channel_gain)
    total_out = jnp.dot(head_normed, attention_out, preferred_element_type=jnp.float32) + jnp.dot(group_normed, channel_out, preferred_element_type=jnp.float32)
    return total_out.astype(jnp.bfloat16)
```

```python
import jax
import jax.numpy as jnp
from jax import lax
from jax.experimental import pallas as pl
from jax.experimental.pallas import tpu as pltpu
from jax.sharding import Mesh
from jax.sharding import PartitionSpec as P

HEAD = 128
KTAP = 3
LOG2E = 1.4426950408889634
LOW = -1e30
EPS = 1e-06
BF = jnp.bfloat16
F32 = jnp.float32

NZ, NY, NC, NX = 8, 4, 2, 4
OWN = 384
CHUNK = NC * OWN
ROWS = OWN // NX
STAT = 16
SUB = 128


def shifted(a, axis, by):
    n = lax.axis_size(axis)
    return lax.ppermute(a, axis, [(i, (i + by) % n) for i in range(n)])


def dot(a, b):
    return jnp.dot(a, b, preferred_element_type=F32)


def update(q, kv, gate, m, l, acc, masked):
    keys, values = kv[:, :HEAD], kv[:, HEAD:]
    s = lax.dot_general(q, keys, (((1,), (1,)), ((), ())), preferred_element_type=F32)
    n = s.shape[1] // HEAD
    scale = HEAD**-0.5 * LOG2E
    parts = []
    for j in range(n):
        part = s[:, j * HEAD : (j + 1) * HEAD] * scale - gate[:, j * HEAD : (j + 1) * HEAD]
        if masked is not None:
            part = jnp.where(masked(j), part, LOW)
        parts.append(part)
    top = parts[0]
    for part in parts[1:]:
        top = jnp.maximum(top, part)
    m_new = jnp.maximum(m, jnp.max(top, axis=1, keepdims=True))
    alpha = jnp.exp2(m - m_new)
    total = l * alpha
    probs = []
    for part in parts:
        p = jnp.exp2(part - m_new)
        total = total + p
        probs.append(p.astype(BF))
    p_all = jnp.concatenate(probs, axis=1)
    acc_new = acc * alpha + dot(p_all, values)
    return m_new, total, acc_new


def first_kernel(code_ref, q_ref, kv_ref, g_ref, m_ref, l_ref, a_ref):
    tile = pl.program_id(0)
    code = code_ref[tile // NC]
    core = code_ref[NY]
    half = tile % NC
    zidx = code_ref[NY + 1]

    @pl.when(code == 0)
    def _():
        m_ref[...] = jnp.full(m_ref.shape, LOW, F32)
        l_ref[...] = jnp.zeros(l_ref.shape, F32)
        a_ref[...] = jnp.zeros(a_ref.shape, F32)

    def run(diag):
        for r in range(OWN // SUB):
            rows = slice(r * SUB, (r + 1) * SUB)
            masked = None
            if diag:
                first = (half * OWN + core * OWN) % CHUNK + r * SUB

                def masked(j):
                    qpos = first + lax.broadcasted_iota(jnp.int32, (SUB, HEAD), 0)
                    kfirst = (j * HEAD + core * OWN) % CHUNK
                    kpos = kfirst + lax.broadcasted_iota(jnp.int32, (SUB, HEAD), 1)
                    return kpos <= qpos

            zero = jnp.zeros((SUB, HEAD), F32)
            m, l, a = update(
                q_ref[rows], kv_ref[...], g_ref[zidx], jnp.full((SUB, HEAD), LOW, F32), zero, zero, masked
            )
            m_ref[rows] = m
            l_ref[rows] = l
            a_ref[rows] = a

    pl.when(code == 1)(lambda: run(False))
    pl.when(code == 2)(lambda: run(True))


def next_kernel(flag_ref, q_ref, kva_ref, kvb_ref, ga_ref, gb_ref, mi, li, ai, mo, lo, ao):
    mo[...] = mi[...]
    lo[...] = li[...]
    ao[...] = ai[...]

    def run(kv_ref, g_ref, zidx):
        for r in range(OWN // SUB):
            rows = slice(r * SUB, (r + 1) * SUB)
            m, l, a = update(q_ref[rows], kv_ref[...], g_ref[zidx], mo[rows], lo[rows], ao[rows], None)
            mo[rows] = m
            lo[rows] = l
            ao[rows] = a

    pl.when(flag_ref[0] == 1)(lambda: run(kva_ref, ga_ref, flag_ref[2]))
    pl.when(flag_ref[1] == 1)(lambda: run(kvb_ref, gb_ref, flag_ref[3]))


def finish(m, l, acc, out_ref):
    total = jnp.sum(l, axis=1, keepdims=True)
    some = total > 0.0
    safe = jnp.where(some, total, 1.0)
    out = (acc / safe).astype(BF)
    lse = jnp.where(some, m + jnp.log2(safe), LOW)
    row = lax.broadcasted_iota(jnp.int32, (ROWS, HEAD), 0)
    lane = lax.broadcasted_iota(jnp.int32, (ROWS, HEAD), 1)
    for b in range(NX):
        rows = slice(b * ROWS, (b + 1) * ROWS)
        out_ref[0, 0, b, :ROWS, :] = out[rows]
        line = jnp.sum(jnp.where(row == lane, lse[rows], 0.0), axis=0, keepdims=True)
        high = line.astype(BF)
        rest = line - high.astype(F32)
        mid = rest.astype(BF)
        low = (rest - mid.astype(F32)).astype(BF)
        out_ref[0, 0, b, ROWS:, :] = jnp.concatenate(
            [high.astype(F32), mid.astype(F32), low.astype(F32), jnp.zeros((STAT - 3, HEAD), F32)], axis=0
        ).astype(BF)


def last_kernel(flag_ref, q_ref, kva_ref, kvb_ref, ga_ref, gb_ref, mi, li, ai, out_ref, mo, lo, ao):
    next_kernel(flag_ref, q_ref, kva_ref, kvb_ref, ga_ref, gb_ref, mi, li, ai, mo, lo, ao)
    finish(mo[...], lo[...], ao[...], out_ref)


def attention_cost(keys):
    rows = NY * CHUNK
    return pl.CostEstimate(
        flops=rows * keys * HEAD * 4, transcendentals=rows * keys, bytes_accessed=rows * HEAD * 26
    )


STATE = jax.ShapeDtypeStruct((NY * CHUNK, HEAD), F32)
TILES = NY * CHUNK // OWN


def tile_spec():
    return pl.BlockSpec((OWN, HEAD), lambda i, *_: (i, 0))


def whole(a):
    return pl.BlockSpec(a.shape, lambda i, *_, n=a.ndim: (0,) * n)


def attend_first(code, q, kv, gate):
    return pl.pallas_call(
        first_kernel,
        grid_spec=pltpu.PrefetchScalarGridSpec(
            num_scalar_prefetch=1,
            grid=(TILES,),
            in_specs=[tile_spec(), whole(kv), whole(gate)],
            out_specs=[tile_spec()] * 3,
        ),
        out_shape=[STATE] * 3,
        cost_estimate=attention_cost(CHUNK),
        name="attend_first",
    )(code, q, kv, gate)


def attend_next(flags, q, kva, kvb, ga, gb, state):
    return pl.pallas_call(
        next_kernel,
        grid_spec=pltpu.PrefetchScalarGridSpec(
            num_scalar_prefetch=1,
            grid=(TILES,),
            in_specs=[tile_spec(), whole(kva), whole(kvb), whole(ga), whole(gb)] + [tile_spec()] * 3,
            out_specs=[tile_spec()] * 3,
        ),
        out_shape=[STATE] * 3,
        input_output_aliases={6: 0, 7: 1, 8: 2},
        cost_estimate=attention_cost(CHUNK),
        name="attend_next",
    )(flags, q, kva, kvb, ga, gb, *state)


def attend_last(flags, q, kva, kvb, ga, gb, state):
    block = (1, 1, NX, ROWS + STAT, HEAD)

    def placed(i, flags):
        return (flags[4 + i // NC], flags[8 + i % NC], 0, 0, 0)

    return pl.pallas_call(
        last_kernel,
        grid_spec=pltpu.PrefetchScalarGridSpec(
            num_scalar_prefetch=1,
            grid=(TILES,),
            in_specs=[tile_spec(), whole(kva), whole(kvb), whole(ga), whole(gb)] + [tile_spec()] * 3,
            out_specs=pl.BlockSpec(block, placed),
            scratch_shapes=[pltpu.VMEM((OWN, HEAD), F32)] * 3,
        ),
        out_shape=jax.ShapeDtypeStruct((NY, NC, NX, ROWS + STAT, HEAD), BF),
        cost_estimate=attention_cost(CHUNK),
        name="attend_last",
    )(flags, q, kva, kvb, ga, gb, *state)


def merge_kernel(where_ref, part_ref, gain_ref, out_ref):
    row = lax.broadcasted_iota(jnp.int32, (ROWS, HEAD), 0)
    lane = lax.broadcasted_iota(jnp.int32, (ROWS, HEAD), 1)
    for c in range(NC):
        sums, outs = [], []
        for y in range(NY):
            stats = part_ref[y, c, 0, ROWS:, :].astype(F32)
            line = stats[0:1] + stats[1:2] + stats[2:3]
            sums.append(jnp.sum(jnp.where(row == lane, line, 0.0), axis=1, keepdims=True))
            outs.append(part_ref[y, c, 0, :ROWS, :].astype(F32))
        top = jnp.maximum(jnp.maximum(sums[0], sums[1]), jnp.maximum(sums[2], sums[3]))
        weights = [jnp.exp2(s - top) for s in sums]
        total = weights[0] + weights[1] + weights[2] + weights[3]
        mixed = (
            outs[0] * weights[0] + outs[1] * weights[1] + outs[2] * weights[2] + outs[3] * weights[3]
        ) / total
        mixed = mixed * lax.rsqrt(jnp.mean(mixed * mixed, axis=1, keepdims=True) + EPS)
        gain = gain_ref[0, 0:1, c * HEAD : (c + 1) * HEAD].astype(F32)
        out_ref[0, :, c * HEAD : (c + 1) * HEAD] = (mixed * gain).astype(BF)


def merge(where, parts, gains):
    return pl.pallas_call(
        merge_kernel,
        grid_spec=pltpu.PrefetchScalarGridSpec(
            num_scalar_prefetch=1,
            grid=(NX,),
            in_specs=[
                pl.BlockSpec((NY, NC, 1, ROWS + STAT, HEAD), lambda i, w: (0, 0, w[i], 0, 0)),
                pl.BlockSpec((1, STAT, NC * HEAD), lambda i, w: (i, 0, 0)),
            ],
            out_specs=pl.BlockSpec((1, ROWS, NC * HEAD), lambda i, w: (i, 0, 0)),
        ),
        out_shape=jax.ShapeDtypeStruct((NX, ROWS, NC * HEAD), BF),
        name="merge",
    )(where, parts, gains)


def group_norm(values, gain):
    count = values.shape[0]
    shaped = values.reshape(count, -1, HEAD)
    shaped = shaped * lax.rsqrt(jnp.mean(shaped * shaped, axis=-1, keepdims=True) + EPS)
    return (shaped.reshape(count, -1) * gain.astype(F32)).astype(BF)


def local(
    tokens, query_weight, key_weight, value_weight, outer_gate, inner_gate, conv_weight, conv_taps,
    gate_sum, head_gain, channel_gain, attention_out, channel_out,
):
    z, y, c, x = (lax.axis_index(a) for a in "zycx")
    other = 1 - c

    def head_of(weight, core):
        return lax.dynamic_slice_in_dim(weight, core * HEAD, HEAD, 1)

    from_left = shifted(tokens, "x", 1)
    from_right = shifted(tokens, "x", -1)
    half = ROWS // 2
    far_top = shifted(from_left[:half], "x", 1)
    far_low = shifted(from_right[half:], "x", -1)
    attn_weights = jnp.concatenate(
        [head_of(w, core) for core in (c, other) for w in (query_weight, key_weight, value_weight)], axis=1
    )
    conv_weights = jnp.concatenate([outer_gate, inner_gate, conv_weight], axis=1)
    pieces = [tokens, jnp.concatenate([from_left, from_right]), jnp.concatenate([far_top, far_low])]
    places = [[x], [(x + NX - 1) % NX, (x + 1) % NX], [(x + 2) % NX]]

    def project(weights):
        rows = jnp.zeros((NX, ROWS, weights.shape[1]), BF)
        for piece, at in zip(pieces, places):
            made = dot(piece, weights).astype(BF)
            for n, place in enumerate(at):
                rows = lax.dynamic_update_slice(rows, made[None, n * ROWS : (n + 1) * ROWS], (place, 0, 0))
        return rows.reshape(OWN, weights.shape[1])

    attn = project(attn_weights)
    mine = attn[:, : 3 * HEAD]
    got = shifted(attn[:, 3 * HEAD :], "c", 1)
    both = jnp.concatenate([mine, got], axis=0)
    q_own, kv_own = both[:, :HEAD], both[:, HEAD:]

    up, down = [kv_own], [kv_own]
    for _ in range(3):
        up.append(shifted(up[-1], "z", 1))
        down.append(shifted(down[-1], "z", -1))
    up_half = shifted(up[3][:OWN], "z", 1)
    down_half = shifted(down[3][OWN:], "z", -1)
    q_all = jnp.concatenate([q_own, shifted(q_own, "y", 1), shifted(q_own, "y", -1), shifted(q_own, "y", 2)])
    slots = jnp.stack([y, (y + NY - 1) % NY, (y + 1) % NY, (y + 2) % NY])

    gate = lax.dynamic_slice_in_dim(gate_sum, c, 1, 0).reshape(NZ, NY, NC, OWN)
    gate = lax.dynamic_index_in_dim(gate, y, 1, keepdims=False)
    gate = jnp.concatenate(
        [lax.dynamic_index_in_dim(gate, c, 1, keepdims=False), lax.dynamic_index_in_dim(gate, other, 1, keepdims=False)],
        axis=1,
    )
    gate = (gate * LOG2E)[:, None, :]

    code = jnp.concatenate([jnp.where(slots == y, 2, jnp.where(slots > y, 1, 0)), jnp.stack([c, z])]).astype(jnp.int32)
    state = attend_first(code, q_all, kv_own, gate)
    cores = jnp.stack([c, other])

    def flags_of(step):
        return jnp.concatenate(
            [
                jnp.stack([(z >= step).astype(jnp.int32), (z + step >= NZ).astype(jnp.int32)]),
                jnp.stack([(z + NZ - step) % NZ, (z + step) % NZ]),
                slots,
                cores,
            ]
        ).astype(jnp.int32)

    for step in range(1, 4):
        state = attend_next(flags_of(step), q_all, up[step], down[step], gate, gate, state)
    partial = attend_last(
        flags_of(4), q_all, up_half, down_half, gate[:, :, :OWN], gate[:, :, OWN:], state
    )

    conv = project(conv_weights)
    width = outer_gate.shape[1]
    gate_outer, gate_inner, conv_input = (conv[:, i * width : (i + 1) * width] for i in range(3))
    mixed_in = (gate_inner.astype(F32) * conv_input.astype(F32)).astype(BF)
    order = ("z", "y", "c")
    count = NZ * NY * NC
    carried = lax.ppermute(mixed_in[OWN - (KTAP - 1) :], order, [(i, i + 1) for i in range(count - 1)])
    padded = jnp.concatenate([carried, mixed_in], axis=0).astype(F32)
    summed = jnp.zeros(mixed_in.shape, F32)
    for offset in range(KTAP):
        summed = summed + conv_taps[offset].astype(F32) * padded[offset : offset + OWN]
    grouped = group_norm(gate_outer.astype(F32) * summed, channel_gain).reshape(NX, ROWS, width)
    gain_rows = jnp.broadcast_to(head_gain[None], (STAT, width))

    def rows_for(place):
        block = lax.dynamic_index_in_dim(grouped, place % NX, 0, keepdims=False)
        return jnp.concatenate([block, gain_rows], axis=0)

    groups = jnp.stack(
        [
            rows_for(x),
            shifted(rows_for(x + 1), "x", 1),
            shifted(rows_for(x + NX - 1), "x", -1),
            shifted(rows_for(x + 2), "x", 2),
        ]
    )
    group_rows, gains = groups[:, :ROWS], groups[:, ROWS:]

    chosen = jnp.where(c == 0, attention_out, channel_out)
    w_left = shifted(chosen, "x", 1)
    w_right = shifted(chosen, "x", -1)
    cut = width // 2
    w_far = (shifted(w_left[:cut], "x", 1), shifted(w_right[cut:], "x", -1))
    first_w = [chosen, w_left, w_right, *w_far]
    second_w = [jnp.where(c == 0, channel_out, attention_out)] + [shifted(w, "c", 1) for w in first_w[1:]]

    parts = partial.reshape(NY * NC * NX, ROWS + STAT, HEAD)
    parts = lax.all_to_all(parts, ("y", "c", "x"), 0, 0, tiled=True)
    where = jnp.stack([x, (x + NX - 1) % NX, (x + 1) % NX, (x + 2) % NX]).astype(jnp.int32)
    heads = merge(where, parts.reshape(NY, NC, NX, ROWS + STAT, HEAD), gains)

    first = jnp.where(c == 0, heads, group_rows)
    second = jnp.where(c == 0, group_rows, heads)
    total = jnp.zeros((ROWS, attention_out.shape[1]), F32)
    for acts, ws in ((first, first_w), (second, second_w)):
        for n in range(3):
            total = total + dot(acts[n], ws[n])
        total = total + dot(acts[3, :, :cut], ws[3]) + dot(acts[3, :, cut:], ws[4])
    return total.astype(BF)


def solution(mesh):
    physical = Mesh(mesh.devices.reshape(NZ, NY, NC, NX), ("z", "y", "c", "x"))
    rows = P(("z", "y", "c", "x"), None)
    cols = P(None, "x")
    placed = (rows,) + (cols,) * 7 + (P("x", None), P("x"), P("x"), P("x", None), P("x", None))
    return jax.shard_map(local, mesh=physical, in_specs=placed, out_specs=rows, check_vma=False)
```
